32 devices in a mesh: ra: 4 (over z), cb: 4 (over y, x), dp: 2 (over core).
Axes of the slice: x: 2, y: 2, z: 4, core: 2. Of those that a mesh axis runs over, the one named last changes fastest.
Arguments:
- tokens: bfloat16 [128, 4096], P('dp', 'ra'), may hold values from -45 to 45
- gain_first: bfloat16 [4096], P('ra'), may hold values from 0.099609375 to 1.8984375
- up_first: float32 [4096, 16384], P('ra', 'cb'), may hold values from -0.125 to 0.125
- up_scale_first: float32 [16384], P('cb'), may hold values from 0.5 to 2
- down_first: float32 [16384, 4096], P('cb', 'ra'), may hold values from -0.046875 to 0.046875
- down_scale_first: float32 [4096], P('ra'), may hold values from 0.5 to 2
- gain_second: bfloat16 [4096], P('ra'), may hold values from 0.099609375 to 1.8984375
- up_second: float32 [4096, 16384], P('ra', 'cb'), may hold values from -0.125 to 0.125
- up_scale_second: float32 [16384], P('cb'), may hold values from 0.5 to 2
- down_second: float32 [16384, 4096], P('cb', 'ra'), may hold values from -0.046875 to 0.046875
- down_scale_second: float32 [4096], P('ra'), may hold values from 0.5 to 2
Outputs:
- mixed_out: bfloat16 [128, 4096], P('dp', 'ra')
The draws below stay inside these ranges and needn't reach their ends.
All inputs are finite; a program needn't handle non-finite values.
Results may differ from the reference program's by a relative error of at most 0.02.
Values may be sent and summed in bfloat16 or wider, within the bound.
A program may use at most 128 MiB of HBM per device.

```python
import math
import jax
import jax.numpy as jnp
from jax import lax

D = 4096
FF = 16384
TOKENS = 128
N_CB = 4


def draw_tokens(key, part):
    key_base = jax.random.fold_in(key, 11)
    key_cols = jax.random.fold_in(key, 12)
    key_rows = jax.random.fold_in(key, 13)
    columns = jnp.arange(D, dtype=jnp.float32) / D
    jitter = jax.random.uniform(key_cols, (D,), jnp.float32, -0.35, 0.35)
    col_scale = jnp.exp(math.log(10.0) * (columns - 0.5) + jitter)
    base = jnp.clip(jax.random.normal(key_base, (TOKENS, D), jnp.float32), -4.0, 4.0)
    row_scale = jnp.exp(jax.random.uniform(key_rows, (TOKENS, 1), jnp.float32, math.log(0.4), math.log(2.5)))
    return (base * row_scale * col_scale[None, :]).astype(jnp.bfloat16)


def strengthened(drawn, own_key, source, target, shards_of, factor):
    owner, partner = [(jnp.arange(drawn.shape[position]) // (drawn.shape[position] // shards_of)).reshape([-1 if axis == position else 1 for axis in range(drawn.ndim)]) for position in (source, target)]
    chosen = jax.random.permutation(own_key, shards_of)[partner]
    strong = (owner == chosen) | (owner == (partner + shards_of // 2) % shards_of)
    return jnp.where(strong, factor * drawn, drawn)


def steps_of(stream_key, extent, cuts, smallest, high):
    def one(dim, shards_of):
        heights = jax.random.uniform(jax.random.fold_in(jax.random.fold_in(stream_key, 6), dim), (shards_of,), jnp.float32, smallest / len(cuts), high / len(cuts))
        return jnp.repeat(jnp.exp(heights), extent[dim] // shards_of).reshape((-1,) + (1,) * (len(extent) - dim - 1))

    loudness = one(*cuts[0])
    for cut in cuts[1:]:
        loudness = loudness * one(*cut)
    return loudness


def bell_draw(key, shape, width, reach, split=(), kind=jnp.bfloat16):
    result = jax.random.normal(key, shape, jnp.float32) * width
    if len(split) > 0:
        result = steps_of(key, shape, split, -0.22, 0.18) * result
    return jnp.clip(result, min=-reach, max=reach).astype(kind)


def gaussian_with(own_key, dims, deviation, most, pieces, heavy, held_as=jnp.bfloat16):
    drawn = deviation * jax.random.normal(own_key, dims, jnp.float32)
    if pieces:
        drawn = drawn * steps_of(own_key, dims, pieces, -0.22, 0.18)
    return jnp.clip(strengthened(drawn, jax.random.fold_in(own_key, 3), *heavy), -most, most).astype(held_as)


def setup_inputs(seed: int = 0) -> dict:
    seeds = jax.random.split(jax.random.key(seed), 12)
    return {
        "tokens": draw_tokens(jax.random.fold_in(seeds[11], 71), 0),
        "gain_first": jnp.clip(1.0 + 0.18 * jax.random.normal(seeds[1], (D,), jnp.float32), 0.099609375, 1.8984375).astype(jnp.bfloat16),
        "up_first": gaussian_with(seeds[2], (D, FF), D ** -0.5, 0.125, ((0, 4), (1, 4)), (0, 1, 4, 2.0), jnp.float32),
        "up_scale_first": jnp.clip(jnp.exp(math.log(2.0) - 1.3862944 * jax.random.uniform(seeds[3], (FF,), jnp.float32) ** steps_of(seeds[3], (FF,), ((0, 4),), -0.2, 0.2)), 0.5, 2.0),
        "down_first": bell_draw(seeds[4], (FF, D), FF ** -0.5, 0.046875, ((0, 4), (1, 4)), jnp.float32),
        "down_scale_first": jnp.clip(jnp.exp(math.log(2.0) - 1.3862944 * jax.random.uniform(seeds[5], (D,), jnp.float32) ** steps_of(seeds[5], (D,), ((0, 4),), -0.2, 0.2)), 0.5, 2.0),
        "gain_second": jnp.clip(1.0 + 0.18 * jax.random.normal(seeds[6], (D,), jnp.float32), 0.099609375, 1.8984375).astype(jnp.bfloat16),
        "up_second": gaussian_with(seeds[7], (D, FF), D ** -0.5, 0.125, ((0, 4), (1, 4)), (0, 1, 4, 2.0), jnp.float32),
        "up_scale_second": jnp.clip(jnp.exp(math.log(2.0) - 1.3862944 * jax.random.uniform(seeds[8], (FF,), jnp.float32) ** steps_of(seeds[8], (FF,), ((0, 4),), -0.2, 0.2)), 0.5, 2.0),
        "down_second": bell_draw(seeds[9], (FF, D), FF ** -0.5, 0.046875, ((0, 4), (1, 4)), jnp.float32),
        "down_scale_second": jnp.clip(jnp.exp(math.log(2.0) - 1.3862944 * jax.random.uniform(seeds[10], (D,), jnp.float32) ** steps_of(seeds[10], (D,), ((0, 4),), -0.2, 0.2)), 0.5, 2.0),
    }


epsilon = 1e-06
residual_share = 0.25

def sub_layer(inputs, norm_gain, up_weight, up_scale, down_weight, down_scale):
    values = inputs.astype(jnp.float32)
    mean_square = lax.optimization_barrier(jnp.mean(values * values, axis=-1, keepdims=True))
    normed = (values * lax.rsqrt(mean_square + epsilon) * norm_gain.astype(jnp.float32)).astype(jnp.bfloat16)
    upward = jnp.dot(normed, up_weight.astype(jnp.bfloat16), preferred_element_type=jnp.float32) * up_scale
    hidden = jnp.square(jax.nn.relu(upward)).astype(jnp.bfloat16)
    down_bf = down_weight.astype(jnp.bfloat16)
    block_rows = hidden.shape[1] // N_CB
    total = jnp.zeros((inputs.shape[0], down_weight.shape[1]), jnp.float32)
    for block in range(N_CB):
        lower = block * block_rows
        part = jnp.dot(hidden[:, lower:lower + block_rows], down_bf[lower:lower + block_rows, :], preferred_element_type=jnp.float32).astype(jnp.bfloat16)
        total = total + lax.optimization_barrier(part).astype(jnp.float32)
    return (residual_share * values + total * down_scale).astype(jnp.bfloat16)

def reference(tokens, gain_first, up_first, up_scale_first, down_first, down_scale_first, gain_second, up_second, up_scale_second, down_second, down_scale_second):
    carried = sub_layer(tokens, gain_first, up_first, up_scale_first, down_first, down_scale_first)
    return sub_layer(carried, gain_second, up_second, up_scale_second, down_second, down_scale_second)
```

```python
import functools

import jax
import jax.numpy as jnp
from jax import lax
from jax.experimental import pallas as pl
from jax.experimental.pallas import tpu as pltpu
from jax.sharding import PartitionSpec as P

epsilon = 1e-06
residual_share = 0.25
MESH = pl.DeviceIdType.MESH
LANES = 128
VMEM_BYTES = 67043328


def visit_order(count):
    return sorted(range(1, count), key=lambda offset: (abs(2 * offset - count), offset))


def fused_kernel(
    plan,
    tokens_ref,
    gain_a,
    up_scale_a,
    down_scale_a,
    gain_b,
    up_scale_b,
    down_scale_b,
    up_a,
    down_a,
    up_b,
    down_b,
    out_ref,
    weights,
    scaled,
    own_partial,
    rs_out,
    rs_in,
    stat_out,
    stat_in,
    hidden_own,
    hidden_in,
    acc,
    part,
    cb_in,
    fresh,
    state,
    w_sem,
    rs_sem,
    stat_sem,
    ag_sem,
    cb_sem,
    cg_sem,
):
    n_ra, n_cb, groups, tile = plan
    gains, up_scales, down_scales = (gain_a, gain_b), (up_scale_a, up_scale_b), (down_scale_a, down_scale_b)
    rows_all, width = tokens_ref.shape
    rows = rows_all // groups
    units = hidden_own.shape[2]
    block = width // n_cb
    full_width = width * n_ra
    r, c = lax.axis_index("ra"), lax.axis_index("cb")
    ra_order, cb_order = visit_order(n_ra), visit_order(n_cb)
    own_columns = pl.ds(pl.multiple_of(c * block, LANES), block)
    sends = []

    def up_copy(layer, j):
        source = (up_a, up_b)[layer]
        buffer = (0, 2)[layer]
        start = pl.multiple_of(lax.rem(r + j, n_ra) * units, LANES)
        return pltpu.make_async_copy(source.at[:, pl.ds(start, units)], weights.at[buffer, j], w_sem.at[2 * layer, j])

    def down_copy(layer, j):
        source = (down_a, down_b)[layer]
        buffer = (1, 0)[layer]
        start = pl.multiple_of(lax.rem(r + n_ra - j, n_ra) * units, LANES)
        return pltpu.make_async_copy(source.at[pl.ds(start, units), :], weights.at[buffer, j], w_sem.at[2 * layer + 1, j])

    up_order = ra_order + [0]
    down_order = [0] + ra_order
    queue = [up_copy(0, j) for j in up_order] + [down_copy(0, j) for j in down_order]
    queue += [up_copy(1, j) for j in up_order]
    issued = [0]

    def issue(count):
        for copy in queue[issued[0] : issued[0] + count]:
            copy.start()
        issued[0] += count

    issue(2)

    barrier = pltpu.get_barrier_semaphore()
    for j in range(1, n_ra):
        pl.semaphore_signal(barrier, inc=1, device_id={"ra": lax.rem(r + j, n_ra)}, device_id_type=MESH)
    for j in range(1, n_cb):
        pl.semaphore_signal(barrier, inc=1, device_id={"cb": lax.rem(c + j, n_cb)}, device_id_type=MESH)

    row_ids = lax.broadcasted_iota(jnp.int32, (rows, LANES), 0)
    lane_ids = lax.broadcasted_iota(jnp.int32, (rows, LANES), 1)
    eye = row_ids == lane_ids

    def send(axis, index, count, j, source, target, sem):
        copy = pltpu.make_async_remote_copy(
            src_ref=source,
            dst_ref=target,
            send_sem=sem.at[0],
            recv_sem=sem.at[1],
            device_id={axis: lax.rem(index + j, count)},
            device_id_type=MESH,
        )
        copy.start()
        sends.append(copy)
        return copy

    stat_copies, rs_copies, ag_copies, cb_copies, cg_copies = {}, {}, {}, {}, {}
    waited = set()

    def span(g):
        return pl.ds(g * rows, rows)

    def prepare(layer, g):
        values = (tokens_ref[span(g), :] if layer == 0 else state[0, span(g), :]).astype(jnp.float32)
        squares = jnp.sum(values * values, axis=1, keepdims=True)
        as_row = jnp.sum(jnp.where(eye, squares, 0.0), axis=0, keepdims=True)
        stat_out[layer, g] = jnp.broadcast_to(as_row, (8, LANES))
        scaled[layer, span(g), :] = (values * gains[layer][...].astype(jnp.float32)).astype(jnp.bfloat16)

    def send_stats(layer, g):
        for j in ra_order:
            stat_copies[layer, g, j] = send(
                "ra", r, n_ra, j, stat_out.at[layer, g], stat_in.at[layer, g, j - 1], stat_sem.at[layer, g, j - 1]
            )

    def wait_weight(kind, layer, j):
        if (kind, layer, j) not in waited:
            waited.add((kind, layer, j))
            (up_copy if kind == "up" else down_copy)(layer, j).wait()
            if kind == "up" and layer == 0:
                issue(1)

    def up_stage(layer, members):
        low, count = members[0] * rows, len(members) * rows
        buffer = (0, 2)[layer]
        for j in up_order:
            wait_weight("up", layer, j)

            def body(i, carry):
                columns = pl.ds(pl.multiple_of(i * tile, LANES), tile)
                value = jnp.dot(
                    scaled[layer, pl.ds(low, count), :],
                    weights[buffer, j, :, columns].astype(jnp.bfloat16),
                    preferred_element_type=jnp.float32,
                )
                if j == 0:
                    own_partial[pl.ds(low, count), columns] = value
                else:
                    rs_out[layer, j - 1, pl.ds(low, count), columns] = value.astype(jnp.bfloat16)
                return carry

            lax.fori_loop(0, units // tile, body, 0)
            if j:
                for g in members:
                    rs_copies[layer, g, j] = send(
                        "ra",
                        r,
                        n_ra,
                        j,
                        rs_out.at[layer, j - 1, span(g), :],
                        rs_in.at[layer, j - 1, span(g), :],
                        rs_sem.at[layer, g, j - 1],
                    )

    def reduce_stage(layer, g):
        total = own_partial[span(g), :]
        squares = stat_out[layer, g]
        for j in ra_order:
            stat_copies[layer, g, j].wait_recv()
            squares = squares + stat_in[layer, g, j - 1]
        as_column = jnp.sum(jnp.where(eye, jnp.broadcast_to(squares[0:1, :], (rows, LANES)), 0.0), axis=1, keepdims=True)
        inverse = lax.rsqrt(as_column / full_width + epsilon)
        for j in ra_order:
            rs_copies[layer, g, j].wait_recv()
            total = total + rs_in[layer, j - 1, span(g), :].astype(jnp.float32)
        scale = up_scales[layer][:, pl.ds(pl.multiple_of(r * units, LANES), units)]
        active = jnp.square(jnp.maximum(total * inverse * scale, 0.0))
        hidden_own[layer, span(g), :] = active.astype(jnp.bfloat16)
        for j in ra_order:
            ag_copies[layer, g, j] = send(
                "ra",
                r,
                n_ra,
                j,
                hidden_own.at[layer, span(g), :],
                hidden_in.at[layer, j - 1, span(g), :],
                ag_sem.at[layer, g, j - 1],
            )

    def down_stage(layer, g):
        buffer = (1, 0)[layer]
        for j in down_order:
            wait_weight("down", layer, j)
            if j:
                ag_copies[layer, g, j].wait_recv()

            def body(i, carry):
                columns = pl.ds(pl.multiple_of(i * tile, LANES), tile)
                source = hidden_own[layer, span(g), :] if j == 0 else hidden_in[layer, j - 1, span(g), :]
                value = jnp.dot(
                    source, weights[buffer, j, :, columns].astype(jnp.bfloat16), preferred_element_type=jnp.float32
                )
                if j == down_order[0]:
                    acc[:, columns] = value
                elif j == down_order[-1]:
                    part[layer, span(g), columns] = (acc[:, columns] + value).astype(jnp.bfloat16)
                else:
                    acc[:, columns] += value
                return carry

            lax.fori_loop(0, width // tile, body, 0)
        for j in cb_order:
            start = pl.multiple_of(lax.rem(c + j, n_cb) * block, LANES)
            cb_copies[layer, g, j] = send(
                "cb",
                c,
                n_cb,
                j,
                part.at[layer, span(g), pl.ds(start, block)],
                cb_in.at[layer, j - 1, span(g), :],
                cb_sem.at[layer, g, j - 1],
            )

    def combine_stage(layer, g):
        total = part[layer, span(g), own_columns].astype(jnp.float32)
        for j in cb_order:
            cb_copies[layer, g, j].wait_recv()
            total = total + cb_in[layer, j - 1, span(g), :].astype(jnp.float32)
        before = (tokens_ref[span(g), own_columns] if layer == 0 else state[0, span(g), own_columns]).astype(jnp.float32)
        after = residual_share * before + total * down_scales[layer][:, own_columns]
        after = after.astype(jnp.bfloat16)
        fresh[layer, span(g), :] = after
        state[layer, span(g), own_columns] = after
        for j in cb_order:
            cg_copies[layer, g, j] = send(
                "cb",
                c,
                n_cb,
                j,
                fresh.at[layer, span(g), :],
                state.at[layer, span(g), own_columns],
                cg_sem.at[layer, g, j - 1],
            )

    def gather_stage(layer, g):
        for j in cb_order:
            cg_copies[layer, g, j].wait_recv()
        if layer == 1:
            out_ref[span(g), :] = state[1, span(g), :]
        else:
            prepare(1, g)
            send_stats(1, g)
            up_stage(1, [g])

    everyone = list(range(groups))
    for g in everyone:
        prepare(0, g)
    pl.semaphore_wait(barrier, n_ra + n_cb - 2)
    for g in everyone:
        send_stats(0, g)
    up_stage(0, everyone)
    issue(len(queue))
    for j in down_order:
        down_copy(1, j).start()
    for layer in range(2):
        for g in everyone:
            reduce_stage(layer, g)
        for g in everyone:
            down_stage(layer, g)
            if g:
                gather_stage(layer, g - 1)
            combine_stage(layer, g)
        gather_stage(layer, groups - 1)
    for copy in sends:
        copy.wait_send()


def fused_shards(
    plan,
    tokens,
    gain_first,
    up_first,
    up_scale_first,
    down_first,
    down_scale_first,
    gain_second,
    up_second,
    up_scale_second,
    down_second,
    down_scale_second,
):
    n_ra, n_cb, groups, _ = plan
    rows_all, width = tokens.shape
    units = up_first.shape[1] // n_ra
    block = width // n_cb
    bf, f32 = jnp.bfloat16, jnp.float32
    small = pl.BlockSpec(memory_space=pltpu.VMEM)
    large = pl.BlockSpec(memory_space=pl.ANY)

    def sems(count):
        return pltpu.SemaphoreType.DMA((2, groups, count - 1, 2))

    return pl.pallas_call(
        functools.partial(fused_kernel, plan),
        out_shape=jax.ShapeDtypeStruct(tokens.shape, tokens.dtype),
        in_specs=[small] * 7 + [large] * 4,
        out_specs=small,
        scratch_shapes=[
            pltpu.VMEM((3, n_ra, width, units), f32),
            pltpu.VMEM((2, rows_all, width), bf),
            pltpu.VMEM((rows_all, units), f32),
            pltpu.VMEM((2, n_ra - 1, rows_all, units), bf),
            pltpu.VMEM((2, n_ra - 1, rows_all, units), bf),
            pltpu.VMEM((2, groups, 8, LANES), f32),
            pltpu.VMEM((2, groups, n_ra - 1, 8, LANES), f32),
            pltpu.VMEM((2, rows_all, units), bf),
            pltpu.VMEM((2, n_ra - 1, rows_all, units), bf),
            pltpu.VMEM((rows_all // groups, width), f32),
            pltpu.VMEM((2, rows_all, width), bf),
            pltpu.VMEM((2, n_cb - 1, rows_all, block), bf),
            pltpu.VMEM((2, rows_all, block), bf),
            pltpu.VMEM((2, rows_all, width), bf),
            pltpu.SemaphoreType.DMA((4, n_ra)),
            sems(n_ra),
            sems(n_ra),
            sems(n_ra),
            sems(n_cb),
            sems(n_cb),
        ],
        compiler_params=pltpu.CompilerParams(collective_id=0, has_side_effects=True, vmem_limit_bytes=VMEM_BYTES),
    )(
        tokens,
        gain_first[None, :],
        up_scale_first[None, :],
        down_scale_first[None, :],
        gain_second[None, :],
        up_scale_second[None, :],
        down_scale_second[None, :],
        up_first,
        down_first,
        up_second,
        down_second,
    )


def plan_for(mesh, d, ff, tokens):
    n_ra, n_cb, n_dp = mesh.shape["ra"], mesh.shape["cb"], mesh.shape["dp"]
    width, units, rows = d // n_ra, ff // (n_cb * n_ra), tokens // n_dp
    if n_ra < 2 or n_cb < 2 or width != units or width % (n_cb * LANES) or rows % 16 or rows > LANES:
        return None
    if 3 * n_ra * width * units * 4 > VMEM_BYTES * 4 // 5:
        return None
    groups = GROUPS if rows % (16 * GROUPS) == 0 else 1
    tile = TILE if width % TILE == 0 else LANES
    return n_ra, n_cb, groups, tile


GROUPS = 2
TILE = 512


def sub_layer(inputs, norm_gain, up_weight, up_scale, down_weight, down_scale):
    values = inputs.astype(jnp.float32)
    full_width = inputs.shape[1] * lax.axis_size("ra")
    squares = lax.psum(jnp.sum(values * values, axis=1, keepdims=True), "ra")
    inverse = lax.rsqrt(squares / full_width + epsilon)
    normed = (values * inverse * norm_gain.astype(jnp.float32)).astype(jnp.bfloat16)
    partial_value = jnp.dot(
        normed, up_weight.astype(jnp.bfloat16), preferred_element_type=jnp.float32
    )
    shares = lax.psum_scatter(partial_value, "ra", scatter_dimension=1, tiled=True)
    share_width = shares.shape[1]
    own_scale = lax.dynamic_slice_in_dim(
        up_scale, lax.axis_index("ra") * share_width, share_width, 0
    )
    own_units = jnp.square(jax.nn.relu(shares * own_scale)).astype(jnp.bfloat16)
    hidden = lax.all_gather(own_units, "ra", axis=1, tiled=True)
    projected = jnp.dot(
        hidden, down_weight.astype(jnp.bfloat16), preferred_element_type=jnp.float32
    ).astype(jnp.bfloat16)
    projected = lax.optimization_barrier(projected).astype(jnp.float32)
    total = lax.psum(projected.astype(jnp.bfloat16), "cb").astype(jnp.float32)
    return (residual_share * values + total * down_scale).astype(jnp.bfloat16)


def shards(
    tokens,
    gain_first,
    up_first,
    up_scale_first,
    down_first,
    down_scale_first,
    gain_second,
    up_second,
    up_scale_second,
    down_second,
    down_scale_second,
):
    carried = sub_layer(tokens, gain_first, up_first, up_scale_first, down_first, down_scale_first)
    return sub_layer(
        carried, gain_second, up_second, up_scale_second, down_second, down_scale_second
    )


def solution(mesh):
    in_specs = (
        P("dp", "ra"),
        P("ra"),
        P("ra", "cb"),
        P("cb"),
        P("cb", "ra"),
        P("ra"),
        P("ra"),
        P("ra", "cb"),
        P("cb"),
        P("cb", "ra"),
        P("ra"),
    )
    out_specs = P("dp", "ra")

    def run(*arrays):
        tokens, up_weight = arrays[0], arrays[2]
        plan = plan_for(mesh, up_weight.shape[0], up_weight.shape[1], tokens.shape[0])
        inner = shards if plan is None else functools.partial(fused_shards, plan)
        mapped = jax.shard_map(inner, mesh=mesh, in_specs=in_specs, out_specs=out_specs, check_vma=False)
        return mapped(*arrays)

    return run
```

```python
import functools

import jax
import jax.numpy as jnp
from jax import lax
from jax.experimental import pallas as pl
from jax.experimental.pallas import tpu as pltpu
from jax.sharding import PartitionSpec as P

epsilon = 1e-06
residual_share = 0.25
MESH = pl.DeviceIdType.MESH
LANES = 128
VMEM_BYTES = 67043328


def visit_order(count):
    return sorted(range(1, count), key=lambda offset: (abs(2 * offset - count), offset))


def fused_kernel(
    plan,
    tokens_ref,
    gain_a,
    up_scale_a,
    down_scale_a,
    gain_b,
    up_scale_b,
    down_scale_b,
    up_a,
    down_a,
    up_b,
    down_b,
    out_ref,
    weights,
    scaled,
    partial,
    rs_out,
    rs_in,
    relay_in,
    stat_out,
    stat_in,
    hidden_own,
    hidden_in,
    acc,
    part,
    cb_in,
    fresh,
    state,
    w_sem,
    rs_sem,
    stat_sem,
    relay_sem,
    ag_sem,
    own_sem,
    cb_sem,
    cg_sem,
):
    n_ra, n_cb, groups, tile = plan
    gains, up_scales, down_scales = (gain_a, gain_b), (up_scale_a, up_scale_b), (down_scale_a, down_scale_b)
    rows_all, width = tokens_ref.shape
    rows = rows_all // groups
    units = hidden_own.shape[2]
    block = width // n_cb
    full_width = width * n_ra
    r, c = lax.axis_index("ra"), lax.axis_index("cb")
    ra_order, cb_order = visit_order(n_ra), visit_order(n_cb)
    own_columns = pl.ds(pl.multiple_of(c * block, LANES), block)
    sends = []

    def up_copy(layer, j):
        source = (up_a, up_b)[layer]
        buffer = (0, 2)[layer]
        start = pl.multiple_of(lax.rem(r + j, n_ra) * units, LANES)
        return pltpu.make_async_copy(source.at[:, pl.ds(start, units)], weights.at[buffer, j], w_sem.at[2 * layer, j])

    def down_copy(layer, j):
        source = (down_a, down_b)[layer]
        buffer = (1, 0)[layer]
        start = pl.multiple_of(lax.rem(r + n_ra - j, n_ra) * units, LANES)
        return pltpu.make_async_copy(source.at[pl.ds(start, units), :], weights.at[buffer, j], w_sem.at[2 * layer + 1, j])

    up_order = ra_order + [0]
    down_order = [0] + sorted(ra_order, key=lambda j: min(j, n_ra - j))
    queue = [up_copy(0, j) for j in up_order] + [down_copy(0, j) for j in down_order]
    queue += [up_copy(1, j) for j in up_order]
    issued = [0]

    def issue(count):
        for copy in queue[issued[0] : issued[0] + count]:
            copy.start()
        issued[0] += count

    issue(2)

    barrier = pltpu.get_barrier_semaphore()
    for j in range(1, n_ra):
        pl.semaphore_signal(barrier, inc=1, device_id={"ra": lax.rem(r + j, n_ra)}, device_id_type=MESH)
    for j in range(1, n_cb):
        pl.semaphore_signal(barrier, inc=1, device_id={"cb": lax.rem(c + j, n_cb)}, device_id_type=MESH)

    row_ids = lax.broadcasted_iota(jnp.int32, (rows, LANES), 0)
    lane_ids = lax.broadcasted_iota(jnp.int32, (rows, LANES), 1)
    eye = row_ids == lane_ids

    def remote(axis, device, source, target, send_sem, recv_sem):
        return pltpu.make_async_remote_copy(
            src_ref=source,
            dst_ref=target,
            send_sem=send_sem,
            recv_sem=recv_sem,
            device_id={axis: device},
            device_id_type=MESH,
        )

    def start_if(condition, copy):
        pl.when(condition)(copy.start)
        sends.append((condition, copy))
        return copy

    def send(axis, index, count, j, source, target, sem):
        copy = remote(axis, lax.rem(index + j, count), source, target, sem.at[0], sem.at[1])
        copy.start()
        sends.append((None, copy))
        return copy

    first, last = r == 0, r == n_ra - 1
    at_end = first | last
    neighbour = jnp.where(first, 1, n_ra - 2)

    def adds_relayed(j):
        low = (r == 1) if j <= n_ra - 2 else False
        high = (r == n_ra - 2) if j >= 2 else False
        return low | high

    def goes_direct(j):
        inner = jnp.logical_not(at_end) & jnp.logical_not(adds_relayed(j))
        if j == 1:
            inner = inner | first
        if j == n_ra - 1:
            inner = inner | last
        return inner

    def goes_to_neighbour(j):
        if j == 1:
            return last
        if j == n_ra - 1:
            return first
        return at_end

    def arrives(j):
        source = lax.rem(r + n_ra - j, n_ra)
        from_first = (source == 0) & (r != 1)
        from_last = (source == n_ra - 1) & (r != n_ra - 2)
        return jnp.logical_not(from_first | from_last)

    stat_copies, rs_copies, cb_copies, cg_copies = {}, {}, {}, {}
    waited = set()

    def span(g):
        return pl.ds(g * rows, rows)

    def prepare(layer, g):
        values = (tokens_ref[span(g), :] if layer == 0 else state[0, span(g), :]).astype(jnp.float32)
        squares = jnp.sum(values * values, axis=1, keepdims=True)
        as_row = jnp.sum(jnp.where(eye, squares, 0.0), axis=0, keepdims=True)
        stat_out[layer, g] = jnp.broadcast_to(as_row, (8, LANES))
        scaled[layer, span(g), :] = (values * gains[layer][...].astype(jnp.float32).reshape(1, width)).astype(jnp.bfloat16)

    def send_stats(layer, g):
        for j in ra_order:
            stat_copies[layer, g, j] = send(
                "ra", r, n_ra, j, stat_out.at[layer, g], stat_in.at[layer, g, j - 1], stat_sem.at[layer, g, j - 1]
            )

    def wait_weight(kind, layer, j):
        if (kind, layer, j) not in waited:
            waited.add((kind, layer, j))
            (up_copy if kind == "up" else down_copy)(layer, j).wait()
            if kind == "up" and layer == 0:
                issue(1)

    def up_stage(layer, members):
        low, count = members[0] * rows, len(members) * rows
        buffer = (0, 2)[layer]
        for j in up_order:
            wait_weight("up", layer, j)

            def body(i, carry):
                columns = pl.ds(pl.multiple_of(i * tile, LANES), tile)
                value = jnp.dot(
                    scaled[layer, pl.ds(low, count), :],
                    weights[buffer, j, :, columns].astype(jnp.bfloat16),
                    preferred_element_type=jnp.float32,
                )
                partial[j, pl.ds(low, count), columns] = value
                if j:
                    rs_out[layer, j - 1, pl.ds(low, count), columns] = value.astype(jnp.bfloat16)
                return carry

            lax.fori_loop(0, units // tile, body, 0)
            if j:
                for g in members:
                    source = rs_out.at[layer, j - 1, span(g), :]
                    target = rs_in.at[layer, j - 1, span(g), :]
                    sem = rs_sem.at[layer, g, j - 1]
                    copy = remote("ra", lax.rem(r + j, n_ra), source, target, sem.at[0], sem.at[1])
                    rs_copies[layer, g, j] = start_if(goes_direct(j), copy)
                    place = jnp.where(first, max(j - 2, 0), min(j, n_ra - 2))
                    target = relay_in.at[layer, place, span(g), :]
                    sem = relay_sem.at[layer, g]
                    copy = remote("ra", neighbour, source, target, sem.at[j - 1, 0], sem.at[place, 1])
                    start_if(goes_to_neighbour(j), copy)

    def relay_stage(layer, g):
        for j in ra_order:

            @pl.when(adds_relayed(j))
            def _():
                sem = relay_sem.at[layer, g, j - 1]
                target = relay_in.at[layer, j - 1, span(g), :]
                remote("ra", neighbour, target, target, sem.at[0], sem.at[1]).wait_recv()
                added = partial[j, span(g), :] + target[...].astype(jnp.float32)
                rs_out[layer, j - 1, span(g), :] = added.astype(jnp.bfloat16)

            start_if(adds_relayed(j), rs_copies[layer, g, j])

    def reduce_stage(layer, g):
        squares = stat_out[layer, g]
        for j in ra_order:
            stat_copies[layer, g, j].wait_recv()
            squares = squares + stat_in[layer, g, j - 1]
        as_column = jnp.sum(jnp.where(eye, jnp.broadcast_to(squares[0:1, :], (rows, LANES)), 0.0), axis=1, keepdims=True)
        inverse = lax.rsqrt(as_column / full_width + epsilon)
        for j in ra_order:

            @pl.when(arrives(j))
            def _():
                rs_copies[layer, g, j].wait_recv()
                partial[0, span(g), :] += rs_in[layer, j - 1, span(g), :].astype(jnp.float32)

        total = partial[0, span(g), :]
        scale = up_scales[layer][:, pl.ds(pl.multiple_of(r * units, LANES), units)]
        active = jnp.square(jnp.maximum(total * inverse * scale, 0.0))
        hidden_own[layer, span(g), :] = active.astype(jnp.bfloat16)
        source = hidden_own.at[layer, span(g), :]
        sem = ag_sem.at[layer, g]
        right = remote("ra", lax.rem(r + 1, n_ra), source, hidden_in.at[layer, 0, span(g), :], own_sem.at[layer, g, 0], sem.at[0, 1])
        left = remote(
            "ra",
            lax.rem(r + n_ra - 1, n_ra),
            source,
            hidden_in.at[layer, n_ra - 2, span(g), :],
            own_sem.at[layer, g, 1],
            sem.at[n_ra - 2, 1],
        )
        start_if(jnp.logical_not(last), right)
        start_if(jnp.logical_not(first), left)

    def take_hidden(layer, g, j):
        sem = ag_sem.at[layer, g]
        source = hidden_in.at[layer, j - 1, span(g), :]
        remote("ra", lax.rem(r + 1, n_ra), source, source, sem.at[j - 1, 0], sem.at[j - 1, 1]).wait_recv()
        if j < n_ra - 1:
            target = hidden_in.at[layer, j, span(g), :]
            copy = remote("ra", lax.rem(r + 1, n_ra), source, target, sem.at[j - 1, 0], sem.at[j, 1])
            start_if((r >= j) & jnp.logical_not(last), copy)
        if j > 1:
            target = hidden_in.at[layer, j - 2, span(g), :]
            copy = remote("ra", lax.rem(r + n_ra - 1, n_ra), source, target, sem.at[j - 1, 0], sem.at[j - 2, 1])
            start_if((r < j) & jnp.logical_not(first), copy)

    def down_stage(layer, g):
        buffer = (1, 0)[layer]
        for j in down_order:
            wait_weight("down", layer, j)
            if j:
                take_hidden(layer, g, j)

            def body(i, carry):
                columns = pl.ds(pl.multiple_of(i * tile, LANES), tile)
                source = hidden_own[layer, span(g), :] if j == 0 else hidden_in[layer, j - 1, span(g), :]
                value = jnp.dot(
                    source, weights[buffer, j, :, columns].astype(jnp.bfloat16), preferred_element_type=jnp.float32
                )
                if j == down_order[0]:
                    acc[:, columns] = value
                elif j == down_order[-1]:
                    part[layer, span(g), columns] = (acc[:, columns] + value).astype(jnp.bfloat16)
                else:
                    acc[:, columns] += value
                return carry

            lax.fori_loop(0, width // tile, body, 0)
        for j in cb_order:
            start = pl.multiple_of(lax.rem(c + j, n_cb) * block, LANES)
            cb_copies[layer, g, j] = send(
                "cb",
                c,
                n_cb,
                j,
                part.at[layer, span(g), pl.ds(start, block)],
                cb_in.at[layer, j - 1, span(g), :],
                cb_sem.at[layer, g, j - 1],
            )

    def combine_stage(layer, g):
        total = part[layer, span(g), own_columns].astype(jnp.float32)
        for j in cb_order:
            cb_copies[layer, g, j].wait_recv()
            total = total + cb_in[layer, j - 1, span(g), :].astype(jnp.float32)
        before = (tokens_ref[span(g), own_columns] if layer == 0 else state[0, span(g), own_columns]).astype(jnp.float32)
        after = residual_share * before + total * down_scales[layer][:, own_columns]
        after = after.astype(jnp.bfloat16)
        fresh[layer, span(g), :] = after
        state[layer, span(g), own_columns] = after
        for j in cb_order:
            cg_copies[layer, g, j] = send(
                "cb",
                c,
                n_cb,
                j,
                fresh.at[layer, span(g), :],
                state.at[layer, span(g), own_columns],
                cg_sem.at[layer, g, j - 1],
            )

    def gather_stage(layer, g):
        for j in cb_order:
            cg_copies[layer, g, j].wait_recv()
        if layer == 1:
            out_ref[span(g), :] = state[1, span(g), :]
        else:
            prepare(1, g)
            send_stats(1, g)
            up_stage(1, [g])

    everyone = list(range(groups))
    for g in everyone:
        prepare(0, g)
    pl.semaphore_wait(barrier, n_ra + n_cb - 2)
    for g in everyone:
        send_stats(0, g)
    up_stage(0, everyone)
    issue(len(queue))
    for j in down_order:
        down_copy(1, j).start()
    for layer in range(2):
        if layer == 0:
            for g in everyone:
                relay_stage(layer, g)
        for stage in (reduce_stage, down_stage, combine_stage):
            for g in everyone:
                stage(layer, g)
        for g in everyone:
            gather_stage(layer, g)
            if layer == 0:
                if g:
                    relay_stage(1, g - 1)
                if g == groups - 1:
                    relay_stage(1, g)
    for condition, copy in sends:
        if condition is None:
            copy.wait_send()
        else:
            pl.when(condition)(copy.wait_send)


def fused_shards(
    plan,
    tokens,
    gain_first,
    up_first,
    up_scale_first,
    down_first,
    down_scale_first,
    gain_second,
    up_second,
    up_scale_second,
    down_second,
    down_scale_second,
):
    n_ra, n_cb, groups, _ = plan
    rows_all, width = tokens.shape
    units = up_first.shape[1] // n_ra
    block = width // n_cb
    bf, f32 = jnp.bfloat16, jnp.float32
    small = pl.BlockSpec(memory_space=pltpu.VMEM)
    large = pl.BlockSpec(memory_space=pl.ANY)

    def sems(count):
        return pltpu.SemaphoreType.DMA((2, groups, count - 1, 2))

    return pl.pallas_call(
        functools.partial(fused_kernel, plan),
        out_shape=jax.ShapeDtypeStruct(tokens.shape, tokens.dtype),
        in_specs=[small] * 7 + [large] * 4,
        out_specs=small,
        scratch_shapes=[
            pltpu.VMEM((3, n_ra, width, units), f32),
            pltpu.VMEM((2, rows_all, width), bf),
            pltpu.VMEM((n_ra, rows_all, units), f32),
            pltpu.VMEM((2, n_ra - 1, rows_all, units), bf),
            pltpu.VMEM((2, n_ra - 1, rows_all, units), bf),
            pltpu.VMEM((2, n_ra - 1, rows_all, units), bf),
            pltpu.VMEM((2, groups, 8, LANES), f32),
            pltpu.VMEM((2, groups, n_ra - 1, 8, LANES), f32),
            pltpu.VMEM((2, rows_all, units), bf),
            pltpu.VMEM((2, n_ra - 1, rows_all, units), bf),
            pltpu.VMEM((rows_all // groups, width), f32),
            pltpu.VMEM((2, rows_all, width), bf),
            pltpu.VMEM((2, n_cb - 1, rows_all, block), bf),
            pltpu.VMEM((2, rows_all, block), bf),
            pltpu.VMEM((2, rows_all, width), bf),
            pltpu.SemaphoreType.DMA((4, n_ra)),
            sems(n_ra),
            sems(n_ra),
            sems(n_ra),
            sems(n_ra),
            pltpu.SemaphoreType.DMA((2, groups, 2)),
            sems(n_cb),
            sems(n_cb),
        ],
        compiler_params=pltpu.CompilerParams(collective_id=0, has_side_effects=True, vmem_limit_bytes=VMEM_BYTES),
    )(
        tokens,
        gain_first,
        up_scale_first[None, :],
        down_scale_first[None, :],
        gain_second,
        up_scale_second[None, :],
        down_scale_second[None, :],
        up_first,
        down_first,
        up_second,
        down_second,
    )


def plan_for(mesh, d, ff, tokens):
    n_ra, n_cb, n_dp = mesh.shape["ra"], mesh.shape["cb"], mesh.shape["dp"]
    width, units, rows = d // n_ra, ff // (n_cb * n_ra), tokens // n_dp
    if n_ra < 4 or n_cb < 2 or width != units or width % (n_cb * LANES) or rows % 16 or rows > LANES:
        return None
    if 3 * n_ra * width * units * 4 > VMEM_BYTES * 4 // 5:
        return None
    groups = GROUPS if rows % (16 * GROUPS) == 0 else 1
    tile = TILE if width % TILE == 0 else LANES
    return n_ra, n_cb, groups, tile


GROUPS = 2
TILE = 512


def sub_layer(inputs, norm_gain, up_weight, up_scale, down_weight, down_scale):
    values = inputs.astype(jnp.float32)
    full_width = inputs.shape[1] * lax.axis_size("ra")
    squares = lax.psum(jnp.sum(values * values, axis=1, keepdims=True), "ra")
    inverse = lax.rsqrt(squares / full_width + epsilon)
    normed = (values * inverse * norm_gain.astype(jnp.float32)).astype(jnp.bfloat16)
    partial_value = jnp.dot(
        normed, up_weight.astype(jnp.bfloat16), preferred_element_type=jnp.float32
    )
    shares = lax.psum_scatter(partial_value, "ra", scatter_dimension=1, tiled=True)
    share_width = shares.shape[1]
    own_scale = lax.dynamic_slice_in_dim(
        up_scale, lax.axis_index("ra") * share_width, share_width, 0
    )
    own_units = jnp.square(jax.nn.relu(shares * own_scale)).astype(jnp.bfloat16)
    hidden = lax.all_gather(own_units, "ra", axis=1, tiled=True)
    projected = jnp.dot(
        hidden, down_weight.astype(jnp.bfloat16), preferred_element_type=jnp.float32
    ).astype(jnp.bfloat16)
    projected = lax.optimization_barrier(projected).astype(jnp.float32)
    total = lax.psum(projected.astype(jnp.bfloat16), "cb").astype(jnp.float32)
    return (residual_share * values + total * down_scale).astype(jnp.bfloat16)


def shards(
    tokens,
    gain_first,
    up_first,
    up_scale_first,
    down_first,
    down_scale_first,
    gain_second,
    up_second,
    up_scale_second,
    down_second,
    down_scale_second,
):
    carried = sub_layer(tokens, gain_first, up_first, up_scale_first, down_first, down_scale_first)
    return sub_layer(
        carried, gain_second, up_second, up_scale_second, down_second, down_scale_second
    )


def solution(mesh):
    in_specs = (
        P("dp", "ra"),
        P("ra"),
        P("ra", "cb"),
        P("cb"),
        P("cb", "ra"),
        P("ra"),
        P("ra"),
        P("ra", "cb"),
        P("cb"),
        P("cb", "ra"),
        P("ra"),
    )
    out_specs = P("dp", "ra")

    def run(*arrays):
        tokens, up_weight = arrays[0], arrays[2]
        plan = plan_for(mesh, up_weight.shape[0], up_weight.shape[1], tokens.shape[0])
        inner = shards if plan is None else functools.partial(fused_shards, plan)
        mapped = jax.shard_map(inner, mesh=mesh, in_specs=in_specs, out_specs=out_specs, check_vma=False)
        return mapped(*arrays)

    return run
```
